32 devices in a mesh: rep: 2 (over x), fs: 8 (over z, y), tp: 2 (over core).
Axes of the slice: x: 2, y: 2, z: 4, core: 2. Of those that a mesh axis runs over, the one named last changes fastest.
Arguments:
- inputs_next: bfloat16 [2048, 2048], P(('rep', 'fs'), 'tp'), parts along dimension 0, may hold values from -6 to 6
- inputs_prev: bfloat16 [2048, 2048], P(('rep', 'fs'), 'tp'), parts along dimension 0, may hold values from -6 to 6
- hidden_prev: bfloat16 [2048, 8192], P(('rep', 'fs')), parts along dimension 0, may hold values from -6 to 6
- cotangent: bfloat16 [2048, 2048], P(('rep', 'fs'), 'tp'), parts along dimension 0, may hold values from -6 to 6
- up_weight: bfloat16 [2048, 8192], P('tp', 'fs'), may hold values from -0.125 to 0.125
- down_weight: bfloat16 [8192, 2048], P('fs', 'tp'), may hold values from -0.0625 to 0.0625
- up_accum: float32 [4096, 8192], P(('rep', 'tp'), 'fs'), parts along dimension 0, may hold values from -192 to 192
- down_accum: float32 [16384, 2048], P(('rep', 'fs'), 'tp'), parts along dimension 0, may hold values from -192 to 192
Outputs:
- output_next: bfloat16 [2048, 2048], P(('rep', 'fs'), 'tp'), parts along dimension 0
- hidden_next: bfloat16 [2048, 8192], P(('rep', 'fs')), parts along dimension 0
- input_grad: bfloat16 [2048, 2048], P(('rep', 'fs'), 'tp'), parts along dimension 0
- up_accum_out: float32 [4096, 8192], P(('rep', 'tp'), 'fs'), parts along dimension 0
- down_accum_out: float32 [16384, 2048], P(('rep', 'fs'), 'tp'), parts along dimension 0
The draws below stay inside these ranges and needn't reach their ends.
There are 2 independent parts, one for each index of `rep`. The reference program is written for one: setup_inputs(seed, part) draws one part's arguments, and reference() takes and returns one part's arrays. A program takes and returns all parts, laid end to end along the dimension named above; an argument that names none is the same for every part. Nothing has to cross between parts.
All inputs are finite; a program needn't handle non-finite values.
Results may differ from the reference program's by a relative error of at most 0.034.
Values may be sent and summed in bfloat16 or wider, within the bound.
No kernel may reach another device: no remote copies, remote signals or barrier semaphores. Data moves between devices by JAX's collectives and lax.ppermute only.
A program may use at most 128 MiB of HBM per device.

```python
import jax
import jax.numpy as jnp

D = 2048
FF = 8192
TOKENS = 1024
N_TP = 2


def with_spikes(drawn, rng, source, target, blocks, factor):
    owner, partner = [(jnp.arange(drawn.shape[axis_at]) // (drawn.shape[axis_at] // blocks)).reshape([-1 if axis == axis_at else 1 for axis in range(drawn.ndim)]) for axis_at in (source, target)]
    chosen = jax.random.permutation(rng, blocks)[partner]
    strong = (owner == chosen) | (owner == (partner + blocks // 2) % blocks)
    return jnp.where(strong, factor * drawn, drawn)


def level_of(rng, dims, shards, low, largest):
    loudness = 1.0
    for position, shards_of in shards:
        heights = jax.random.uniform(jax.random.fold_in(jax.random.fold_in(rng, 6), position), (shards_of,), jnp.float32, low / len(shards), largest / len(shards))
        loudness = loudness * jnp.repeat(jnp.exp(heights), dims[position] // shards_of).reshape((-1,) + (1,) * (len(dims) - 1 - position))
    return loudness


def centred(own_key, dims, scale, most, split=(), held_as=jnp.bfloat16):
    level = level_of(own_key, dims, split, -0.22, 0.18) if split else 1.0
    values = jax.random.normal(own_key, dims, jnp.float32) * scale * level
    return jnp.minimum(jnp.maximum(values, -most), most).astype(held_as)


def heavy_noise(key, shape, deviation, reach, pieces, heavy, kind=jnp.bfloat16):
    drawn = deviation * jax.random.normal(key, shape, jnp.float32)
    if pieces:
        drawn = drawn * level_of(key, shape, pieces, -0.22, 0.18)
    return jnp.clip(with_spikes(drawn, jax.random.fold_in(key, 3), *heavy), -reach, reach).astype(kind)


def setup_inputs(seed: int = 0, part: int = 0) -> dict:
    splits = jax.random.split(jax.random.key(seed), 9)
    part_splits = jax.random.split(jax.random.fold_in(splits[8], part), 9)
    inputs_next = centred(part_splits[0], (TOKENS, D), 1.0, 6.0, ((0, 8), (1, 2)))
    inputs_prev = centred(part_splits[1], (TOKENS, D), 1.0, 6.0, ((0, 8), (1, 2)))
    hidden_prev = centred(part_splits[2], (TOKENS, FF), 1.0, 6.0, ((0, 8),))
    cotangent = heavy_noise(part_splits[3], (TOKENS, D), 1.0, 6.0, ((0, 8), (1, 2)), (0, 1, 8, 2.0))
    up_weight = centred(splits[4], (D, FF), D ** -0.5, 0.125, ((0, 2), (1, 8)))
    down_weight = centred(splits[5], (FF, D), FF ** -0.5, 0.0625, ((0, 8), (1, 2)))
    up_accum = centred(part_splits[6], (D, FF), 32.0, 192.0, ((0, 2), (1, 8)), jnp.float32)
    down_accum = centred(part_splits[7], (FF, D), 32.0, 192.0, ((0, 8), (1, 2)), jnp.float32)
    return {"inputs_next": inputs_next, "inputs_prev": inputs_prev, "hidden_prev": hidden_prev, "cotangent": cotangent, "up_weight": up_weight, "down_weight": down_weight, "up_accum": up_accum, "down_accum": down_accum}


def squared_relu(values):
    return jnp.square(jax.nn.relu(values.astype(jnp.float32))).astype(jnp.bfloat16)


def reference(inputs_next, inputs_prev, hidden_prev, cotangent, up_weight, down_weight, up_accum, down_accum):
    col_width = D // N_TP
    row_total = inputs_next.shape[0]
    hidden_total = jnp.zeros((row_total, FF), jnp.float32)
    back_total = jnp.zeros((row_total, FF), jnp.float32)
    for block_index in range(N_TP):
        start_col = block_index * col_width
        partial_value = jnp.dot(inputs_next[:, start_col:start_col + col_width], up_weight[start_col:start_col + col_width, :], preferred_element_type=jnp.float32)
        hidden_total = hidden_total + partial_value.astype(jnp.bfloat16).astype(jnp.float32)
        backward = jnp.dot(cotangent[:, start_col:start_col + col_width], down_weight[:, start_col:start_col + col_width].T, preferred_element_type=jnp.float32)
        back_total = back_total + backward.astype(jnp.bfloat16).astype(jnp.float32)
    hidden_next = hidden_total.astype(jnp.bfloat16)
    acts_next = squared_relu(hidden_next)
    output_next = jnp.dot(acts_next, down_weight, preferred_element_type=jnp.float32).astype(jnp.bfloat16)
    hidden_saved = hidden_prev.astype(jnp.float32)
    acts_prev = squared_relu(hidden_prev)
    hidden_grad = (back_total * 2.0 * jax.nn.relu(hidden_saved)).astype(jnp.bfloat16)
    input_grad = jnp.dot(hidden_grad, up_weight.T, preferred_element_type=jnp.float32).astype(jnp.bfloat16)
    up_accum_out = up_accum + jnp.dot(inputs_prev.T, hidden_grad, preferred_element_type=jnp.float32)
    down_accum_out = down_accum + jnp.dot(acts_prev.T, cotangent, preferred_element_type=jnp.float32)
    return (output_next, hidden_next, input_grad, up_accum_out, down_accum_out)
```

```python
import jax
import jax.numpy as jnp
from jax import lax
from jax.sharding import PartitionSpec as P


def squared_relu(values):
    return jnp.square(jax.nn.relu(values.astype(jnp.float32))).astype(jnp.bfloat16)


def contract(left, right, left_dim, right_dim):
    return lax.dot_general(
        left, right, (((left_dim,), (right_dim,)), ((), ())), preferred_element_type=jnp.float32
    )


def total_over_tp(terms, n_tp):
    if n_tp == 2:
        theirs = lax.ppermute(terms, "tp", [(0, 1), (1, 0)])
        return terms.astype(jnp.float32) + theirs.astype(jnp.float32)
    return lax.psum(terms, "tp").astype(jnp.float32)


def join_over_tp(part, n_tp):
    if n_tp == 2:
        theirs = lax.ppermute(part, "tp", [(0, 1), (1, 0)])
        first = lax.axis_index("tp") == 0
        return jnp.stack(
            [jnp.where(first, part, theirs), jnp.where(first, theirs, part)], axis=part.ndim - 1
        )
    return lax.all_gather(part, "tp", axis=part.ndim - 1, tiled=False)


def make_local(n_fs, n_tp):
    def local(
        inputs_next, inputs_prev, hidden_prev, cotangent, up_weight, down_weight, up_accum, down_accum
    ):
        me_tp = lax.axis_index("tp")
        rows, ff = hidden_prev.shape
        units = ff // n_fs
        piece = units // n_tp

        def gather(x):
            return lax.all_gather(x, "fs", axis=0, tiled=True)

        inputs_all = gather(inputs_next)
        cotangent_all = gather(cotangent)
        saved_inputs = gather(inputs_prev)

        saved_mine = lax.dynamic_slice_in_dim(
            hidden_prev.reshape(rows, n_fs, n_tp, piece), me_tp, 1, axis=2
        ).reshape(rows, n_fs, piece)
        saved_mine = lax.all_to_all(saved_mine, "fs", split_axis=1, concat_axis=0, tiled=True)
        saved_spread = join_over_tp(saved_mine.reshape(n_fs * rows, piece), n_tp)
        saved_spread = saved_spread.reshape(n_fs * rows, units)

        hidden_terms = contract(inputs_all, up_weight, 1, 0).astype(jnp.bfloat16)
        hidden_spread = total_over_tp(hidden_terms, n_tp).astype(jnp.bfloat16)
        hidden_mine = lax.dynamic_slice_in_dim(hidden_spread, me_tp * piece, piece, axis=1)
        hidden_mine = lax.all_to_all(
            hidden_mine.reshape(n_fs, rows, piece), "fs", split_axis=0, concat_axis=0, tiled=True
        )
        hidden_next = join_over_tp(hidden_mine, n_tp)
        hidden_next = jnp.transpose(hidden_next, (1, 0, 2, 3)).reshape(rows, ff)
        output_terms = contract(squared_relu(hidden_spread), down_weight, 1, 0).astype(jnp.bfloat16)
        output_next = lax.psum_scatter(output_terms, "fs", scatter_dimension=0, tiled=True)

        back_terms = contract(cotangent_all, down_weight, 1, 1).astype(jnp.bfloat16)
        back_sum = total_over_tp(back_terms, n_tp)
        grad_spread = (back_sum * 2.0 * jax.nn.relu(saved_spread.astype(jnp.float32))).astype(
            jnp.bfloat16
        )
        input_terms = contract(grad_spread, up_weight, 1, 1).astype(jnp.bfloat16)
        input_grad = lax.psum_scatter(input_terms, "fs", scatter_dimension=0, tiled=True)
        down_accum_out = down_accum + contract(squared_relu(saved_spread), cotangent_all, 0, 0)
        up_accum_out = up_accum + contract(saved_inputs, grad_spread, 0, 0)
        return (output_next, hidden_next, input_grad, up_accum_out, down_accum_out)

    return local


def solution(mesh):
    return jax.shard_map(
        make_local(mesh.shape["fs"], mesh.shape["tp"]),
        mesh=mesh,
        in_specs=(
            P(("rep", "fs"), "tp"),
            P(("rep", "fs"), "tp"),
            P(("rep", "fs"), None),
            P(("rep", "fs"), "tp"),
            P("tp", "fs"),
            P("fs", "tp"),
            P(("rep", "tp"), "fs"),
            P(("rep", "fs"), "tp"),
        ),
        out_specs=(
            P(("rep", "fs"), "tp"),
            P(("rep", "fs"), None),
            P(("rep", "fs"), "tp"),
            P(("rep", "tp"), "fs"),
            P(("rep", "fs"), "tp"),
        ),
        check_vma=False,
    )
```

```python
import functools

import jax
import jax.numpy as jnp
from jax import lax
from jax.experimental import pallas as pl
from jax.experimental.pallas import tpu as pltpu
from jax.sharding import PartitionSpec as P


def contract(left, right, left_dim, right_dim):
    return lax.dot_general(
        left, right, (((left_dim,), (right_dim,)), ((), ())), preferred_element_type=jnp.float32
    )


def ring_order(mesh):
    n = mesh.shape["fs"]
    at = mesh.axis_names.index("fs")
    line = [mesh.devices[tuple(i if a == at else 0 for a in range(mesh.devices.ndim))] for i in range(n)]
    width = 2
    spots = [getattr(d, "coords", None) for d in line]
    if n > 2 and all(s is not None for s in spots):
        fast = [c for c in range(3) if spots[0][c] != spots[1][c]]
        if len(fast) == 1:
            width = len({s[fast[0]] for s in spots})
    if n % width or (n // width) % 2:
        width = 2
    order = [row * width for row in range(n // width)]
    for back, row in enumerate(reversed(range(n // width))):
        columns = list(range(1, width))
        order += [row * width + c for c in (columns if back % 2 == 0 else reversed(columns))]
    return order


def add_terms(*terms):
    total = terms[0].astype(jnp.float32)
    for term in terms[1:]:
        total = total + term.astype(jnp.float32)
    return total.astype(jnp.bfloat16)


class Ring:
    def __init__(self, order):
        self.n = n = len(order)
        self.order = order
        self.ahead = [(order[i], order[(i + 1) % n]) for i in range(n)]
        self.behind = [(b, a) for a, b in self.ahead]

    def shift(self, x, k):
        n, order = self.n, self.order
        return lax.ppermute(x, "fs", [(order[i], order[(i + k) % n]) for i in range(n)])

    def places(self):
        n = self.n
        place = [0] * n
        for i, index in enumerate(self.order):
            place[index] = i
        mine = jnp.asarray(place, jnp.int32)[lax.axis_index("fs")]
        return jnp.asarray(self.order, jnp.int32)[(mine + jnp.arange(n, dtype=jnp.int32)) % n]

    def gather(self, x):
        n, half = self.n, x.shape[0] // 2
        blocks = [x] + [None] * (n - 1)
        up = down = x
        for k in range(1, n // 2):
            up = lax.ppermute(up, "fs", self.ahead)
            down = lax.ppermute(down, "fs", self.behind)
            blocks[n - k], blocks[k] = up, down
        blocks[n // 2] = jnp.concatenate(
            [lax.ppermute(up[:half], "fs", self.ahead), lax.ppermute(down[half:], "fs", self.behind)]
        )
        return blocks

    def exchange(self, blocks):
        n = self.n
        return [blocks[0]] + [self.shift(blocks[n - j], n - j) for j in range(1, n)]

    def scatter_sum(self, blocks):
        n = self.n
        far = blocks[n // 2]
        half = far.shape[1] // 2
        up = lax.ppermute(far[:, :half], "fs", self.ahead)
        down = lax.ppermute(far[:, half:], "fs", self.behind)
        for k in range(n // 2 - 1, 0, -1):
            mine_up, mine_down = blocks[k], blocks[n - k]
            if k == n // 2 - 1:
                up = jnp.concatenate([add_terms(mine_up[:, :half], up), mine_up[:, half:]], axis=1)
                down = jnp.concatenate(
                    [mine_down[:, :half], add_terms(mine_down[:, half:], down)], axis=1
                )
            else:
                up, down = add_terms(mine_up, up), add_terms(mine_down, down)
            up = lax.ppermute(up, "fs", self.ahead)
            down = lax.ppermute(down, "fs", self.behind)
        return add_terms(blocks[0], up, down)


def pick_kernel(at_ref, x_ref, o_ref):
    o_ref[...] = x_ref[...]


def pick_columns(x, at, width):
    rows, count = x.shape[0], at.shape[0]
    if width % 128:
        cut = jnp.take(x.reshape(rows, -1, width), at, axis=1)
        return jnp.transpose(cut, (1, 0, 2)).reshape(count * rows, width)
    return pl.pallas_call(
        pick_kernel,
        out_shape=jax.ShapeDtypeStruct((count * rows, width), x.dtype),
        grid_spec=pltpu.PrefetchScalarGridSpec(
            num_scalar_prefetch=1,
            grid=(count,),
            in_specs=[pl.BlockSpec((rows, width), lambda i, at: (0, at[i]))],
            out_specs=pl.BlockSpec((rows, width), lambda i, at: (i, 0)),
        ),
        name="pick_columns",
    )(at, x)


def place_kernel(count, at_ref, *refs):
    o_ref = refs[count]
    for i in range(count):

        @pl.when(pl.program_id(0) == i)
        def _():
            o_ref[...] = refs[i][...]


def place_columns(parts, at, total):
    rows, width = parts[0].shape
    count = len(parts)
    return pl.pallas_call(
        functools.partial(place_kernel, count),
        out_shape=jax.ShapeDtypeStruct((rows, total), parts[0].dtype),
        grid_spec=pltpu.PrefetchScalarGridSpec(
            num_scalar_prefetch=1,
            grid=(count,),
            in_specs=[pl.BlockSpec((rows, width), lambda i, at: (0, 0))] * count,
            out_specs=pl.BlockSpec((rows, width), lambda i, at: (0, at[i])),
        ),
        name="place_columns",
    )(at, *parts)


def swap_tp(x):
    return lax.ppermute(x, "tp", [(0, 1), (1, 0)])


def total_over_tp(terms, n_tp):
    if n_tp == 2:
        return terms.astype(jnp.float32) + swap_tp(terms).astype(jnp.float32)
    return lax.psum(terms, "tp").astype(jnp.float32)


def squared_relu(values):
    return jnp.square(jax.nn.relu(values.astype(jnp.float32))).astype(jnp.bfloat16)


def make_local(ring, n_tp):
    n = ring.n

    def local(
        inputs_next, inputs_prev, hidden_prev, cotangent, up_weight, down_weight, up_accum, down_accum
    ):
        me_tp = lax.axis_index("tp")
        rows, ff = hidden_prev.shape
        units = ff // n
        piece = units // n_tp
        places = ring.places()

        def block(x, j):
            return lax.slice_in_dim(x, j * rows, (j + 1) * rows, axis=0)

        inputs_all = jnp.concatenate(ring.gather(inputs_next))
        cotangent_all = jnp.concatenate(ring.gather(cotangent))

        saved_out = pick_columns(hidden_prev, places * n_tp + me_tp, piece)
        saved_mine = jnp.concatenate(ring.exchange([block(saved_out, j) for j in range(n)]))
        if n_tp == 2:
            saved_theirs = swap_tp(saved_mine)
            first = me_tp == 0
            saved = jnp.concatenate(
                [
                    jnp.where(first, saved_mine, saved_theirs),
                    jnp.where(first, saved_theirs, saved_mine),
                ],
                axis=1,
            )
        else:
            saved = lax.all_gather(saved_mine, "tp", axis=1, tiled=True)

        hidden_terms = contract(inputs_all, up_weight, 1, 0).astype(jnp.bfloat16)
        hidden = total_over_tp(hidden_terms, n_tp).astype(jnp.bfloat16)
        hidden_mine = lax.dynamic_slice_in_dim(hidden, me_tp * piece, piece, axis=1)
        hidden_mine = ring.exchange([block(hidden_mine, j) for j in range(n)])
        if n_tp == 2:
            theirs = swap_tp(jnp.concatenate(hidden_mine))
            parts = hidden_mine + [block(theirs, j) for j in range(n)]
            at = jnp.concatenate([places * 2 + me_tp, places * 2 + 1 - me_tp])
        else:
            whole = lax.all_gather(jnp.concatenate(hidden_mine), "tp", axis=0, tiled=True)
            parts = [block(whole, j) for j in range(n * n_tp)]
            at = (places[None, :] * n_tp + jnp.arange(n_tp, dtype=jnp.int32)[:, None]).reshape(-1)
        if piece % 128 == 0:
            hidden_next = place_columns(parts, at, ff)
        else:
            stacked = jnp.stack(parts, axis=1)
            hidden_next = stacked[:, jnp.argsort(at), :].reshape(rows, ff)
        output_terms = contract(squared_relu(hidden), down_weight, 1, 0).astype(jnp.bfloat16)
        output_next = ring.scatter_sum([block(output_terms, j) for j in range(n)])

        back_terms = contract(cotangent_all, down_weight, 1, 1).astype(jnp.bfloat16)
        back_sum = total_over_tp(back_terms, n_tp)
        grad = (back_sum * 2.0 * jax.nn.relu(saved.astype(jnp.float32))).astype(jnp.bfloat16)
        input_terms = contract(grad, up_weight, 1, 1).astype(jnp.bfloat16)
        input_grad = ring.scatter_sum([block(input_terms, j) for j in range(n)])
        down_accum_out = down_accum + contract(squared_relu(saved), cotangent_all, 0, 0)
        saved_inputs = jnp.concatenate(ring.gather(inputs_prev))
        up_accum_out = up_accum + contract(saved_inputs, grad, 0, 0)
        return (output_next, hidden_next, input_grad, up_accum_out, down_accum_out)

    return local


def solution(mesh):
    return jax.shard_map(
        make_local(Ring(ring_order(mesh)), mesh.shape["tp"]),
        mesh=mesh,
        in_specs=(
            P(("rep", "fs"), "tp"),
            P(("rep", "fs"), "tp"),
            P(("rep", "fs"), None),
            P(("rep", "fs"), "tp"),
            P("tp", "fs"),
            P("fs", "tp"),
            P(("rep", "tp"), "fs"),
            P(("rep", "fs"), "tp"),
        ),
        out_specs=(
            P(("rep", "fs"), "tp"),
            P(("rep", "fs"), None),
            P(("rep", "fs"), "tp"),
            P(("rep", "tp"), "fs"),
            P(("rep", "fs"), "tp"),
        ),
        check_vma=False,
    )
```
